32 devices in a mesh: fs: 4 (over z), rep: 4 (over y, x), tp: 2 (over core).
Axes of the slice: x: 2, y: 2, z: 4, core: 2. Of those that a mesh axis runs over, the one named last changes fastest.
Arguments:
- first_mix: bfloat16 [12288, 2048], P(('fs', 'rep'), 'tp'), may hold values from -6 to 6
- second_mix: bfloat16 [12288, 2048], P(('fs', 'rep'), 'tp'), may hold values from -6 to 6
- lambda_head: float32 [8], P('tp'), may hold values from 0.3 to 0.8
- head_gain: float32 [256], replicated, may hold values from 0.1 to 1.9
- out_cotangent: bfloat16 [12288, 2048], P(('fs', 'rep')), may hold values from -0.053955078 to 0.053955078
- basis: bfloat16 [2048, 256], P('tp'), may hold values from -0.125 to 0.125
- weight: float32 [2048, 2048], P('tp', 'fs'), may hold values from -3 to 3
- first_moment: float32 [2048, 256], P('fs', 'tp'), may hold values from -4.5 to 4.5
- second_moment: float32 [2048, 256], P('fs', 'tp'), may hold values from 0.05 to 0.5
Outputs:
- weight_new: float32 [2048, 2048], P('tp', 'fs')
- weight_copy: bfloat16 [2048, 2048], P('tp')
- step_out: float32 [2048, 2048], P('tp', 'fs')
- first_new: float32 [2048, 256], P('fs', 'tp')
- second_new: float32 [2048, 256], P('fs', 'tp')
The draws below stay inside these ranges and needn't reach their ends.
All inputs are finite; a program needn't handle non-finite values.
Results may differ from the reference program's by a relative error of at most 0.0075.
Values may be sent and summed in bfloat16 or wider, within the bound.
A program may use at most 64 MiB of HBM per device.

```python
import math
import jax
import jax.numpy as jnp
from jax import lax

D = 2048
HEADS = 8
HEAD_V = 256
RANK = 256
TOK_DEV = 768
HV = 2048
TOKENS = 12288


def draw_first_moment(key, part):
    draw_base = jnp.clip(jax.random.normal(key, (D, RANK), jnp.float32), -3.0, 3.0)
    roughness = jax.random.uniform(jax.random.fold_in(key, 7), (D, RANK), jnp.float32, 0.5, 1.5)
    rising = 10.0 ** (jnp.arange(D, dtype=jnp.float32) / D)
    return draw_base * 0.1 * rising[:, None] * roughness


def raised(entries, own_key, source, target, parts, factor):
    def block_of(axis_at):
        return (jnp.arange(entries.shape[axis_at]) // (entries.shape[axis_at] // parts)).reshape((-1,) + (1,) * (entries.ndim - 1 - axis_at))

    near = jax.random.permutation(own_key, parts)[block_of(target)]
    second = (block_of(target) + parts // 2) % parts
    return jnp.where((block_of(source) == near) | (block_of(source) == second), factor * entries, entries)


def shard_levels(stream_key, extent, cuts, low, largest):
    def one(axis_at, blocks):
        steps = jax.random.uniform(jax.random.fold_in(jax.random.fold_in(stream_key, 6), axis_at), (blocks,), jnp.float32, low / len(cuts), largest / len(cuts))
        return jnp.repeat(jnp.exp(steps), extent[axis_at] // blocks).reshape((-1,) + (1,) * (len(extent) - axis_at - 1))

    gain = one(*cuts[0])
    for cut in cuts[1:]:
        gain = gain * one(*cut)
    return gain


def bell_draw(stream_key, shape, deviation, limit, cuts=(), kind=jnp.bfloat16):
    loudness = shard_levels(stream_key, shape, cuts, -0.22, 0.18) if cuts else 1.0
    array = jax.random.normal(stream_key, shape, jnp.float32) * deviation * loudness
    return jnp.minimum(jnp.maximum(array, -limit), limit).astype(kind)


def gaussian_with(key, extent, width, most, cuts, heavy, held_as=jnp.bfloat16):
    values = width * jax.random.normal(key, extent, jnp.float32)
    if cuts:
        values = values * shard_levels(key, extent, cuts, -0.22, 0.18)
    return jnp.clip(raised(values, jax.random.fold_in(key, 3), *heavy), -most, most).astype(held_as)


def setup_inputs(seed: int = 0) -> dict:
    splits = jax.random.split(jax.random.key(seed), 10)
    return {
        "first_mix": bell_draw(splits[0], (TOKENS, HV), 1.0, 6.0, ((0, 16), (1, 2))),
        "second_mix": bell_draw(splits[1], (TOKENS, HV), 1.0, 6.0, ((0, 16), (1, 2))),
        "lambda_head": jnp.clip(0.3 + 0.5 * jax.random.uniform(splits[2], (HEADS,), jnp.float32) ** shard_levels(splits[2], (HEADS,), ((0, 2),), -0.2, 0.2), 0.3, 0.8),
        "head_gain": jnp.clip(1.0 + 0.18 * jax.random.normal(splits[3], (HEAD_V,), jnp.float32), 0.1, 1.9),
        "out_cotangent": gaussian_with(splits[4], (TOKENS, D), (TOKENS ** -0.5), 0.053955078, ((0, 16),), (0, 1, 16, 2.0)),
        "basis": bell_draw(splits[5], (HV, RANK), HV ** -0.5, 0.125, ((0, 2),)),
        "weight": bell_draw(splits[6], (HV, D), 0.5, 3.0, ((0, 2), (1, 4)), jnp.float32),
        "first_moment": draw_first_moment(jax.random.fold_in(splits[9], 71), 0),
        "second_moment": jnp.clip(jnp.exp(math.log(0.5) - 2.3025851 * jax.random.uniform(splits[8], (D, RANK), jnp.float32) ** shard_levels(splits[8], (D, RANK), ((0, 4), (1, 2)), -0.2, 0.2)), 0.05, 0.5),
    }


out_scale = 0.8
beta_first = 0.9
beta_second = 0.95

def head_output(first_piece, second_piece, lambdas, head_gain):
    token_count = first_piece.shape[0]
    head_width = head_gain.shape[0]
    head_count = lambdas.shape[0] // head_width
    mixture = first_piece.astype(jnp.float32) - lambdas[None, :] * second_piece.astype(jnp.float32)
    grouped = mixture.reshape(token_count, head_count, head_width)
    inverse = lax.rsqrt(lax.optimization_barrier(jnp.mean(grouped * grouped, axis=-1, keepdims=True)) + 1e-06)
    normed = grouped * inverse * head_gain[None, None, :] * out_scale
    return normed.reshape(token_count, head_count * head_width).astype(jnp.bfloat16)

def reference(first_mix, second_mix, lambda_head, head_gain, out_cotangent, basis, weight, first_moment, second_moment):
    block_count = first_mix.shape[0] // TOK_DEV
    lambdas = jnp.repeat(lambda_head, HEAD_V)

    def accumulate(running, pieces):
        first_piece, second_piece, cot_piece = pieces
        head_out = head_output(first_piece, second_piece, lambdas, head_gain)
        term = lax.dot_general(cot_piece, head_out, (((0,), (0,)), ((), ())), preferred_element_type=jnp.float32)
        return (running + term, None)
    grad_t, _ = lax.scan(accumulate, jnp.zeros((D, HV), jnp.float32), (first_mix.reshape(block_count, TOK_DEV, HV), second_mix.reshape(block_count, TOK_DEV, HV), out_cotangent.reshape(block_count, TOK_DEV, D)))
    basis_wide = basis.astype(jnp.float32)
    projected = jnp.dot(grad_t, basis_wide, precision=lax.Precision.HIGHEST)
    first_new = beta_first * first_moment + (1.0 - beta_first) * projected
    second_new = beta_second * second_moment + (1.0 - beta_second) * projected * projected
    direction = first_new / (jnp.sqrt(second_new) + 1e-08)
    spread = jnp.sqrt(jnp.mean(direction * direction))
    step_out = jnp.dot(basis_wide, direction.T, precision=lax.Precision.HIGHEST) * (-1.0 / (spread + 1e-06))
    weight_new = weight + step_out
    weight_copy = weight_new.astype(jnp.bfloat16)
    return (weight_new, weight_copy, step_out, first_new, second_new)
```

```python
import functools

import jax
import jax.numpy as jnp
from jax import lax
from jax.experimental import pallas as pl
from jax.experimental.pallas import tpu as pltpu
from jax.sharding import PartitionSpec as P

MESH = pl.DeviceIdType.MESH

vmem_grant = 67043328
out_scale = 0.8
beta_first = 0.9
beta_second = 0.95


def head_output(first_piece, second_piece, lambdas, head_gain):
    token_count = first_piece.shape[0]
    head_width = head_gain.shape[0]
    head_count = lambdas.shape[0] // head_width
    mixture = first_piece.astype(jnp.float32) - lambdas[None, :] * second_piece.astype(jnp.float32)
    grouped = mixture.reshape(token_count, head_count, head_width)
    inverse = lax.rsqrt(jnp.mean(grouped * grouped, axis=-1, keepdims=True) + 1e-06)
    normed = grouped * inverse * head_gain[None, None, :] * out_scale
    return normed.reshape(token_count, head_count * head_width).astype(jnp.bfloat16)


def split_product(narrow, wide, numbers):
    upper = wide.astype(jnp.bfloat16)
    lower = (wide - upper.astype(jnp.float32)).astype(jnp.bfloat16)
    return lax.dot_general(
        narrow, upper, numbers, preferred_element_type=jnp.float32
    ) + lax.dot_general(narrow, lower, numbers, preferred_element_type=jnp.float32)


def body(
    first_mix,
    second_mix,
    lambda_head,
    head_gain,
    out_cotangent,
    basis,
    weight,
    first_moment,
    second_moment,
):
    lambdas = jnp.repeat(lambda_head, head_gain.shape[0])
    head_out = head_output(first_mix, second_mix, lambdas, head_gain)
    reduced = jnp.dot(head_out, basis, preferred_element_type=jnp.float32)
    proj_rows = lax.psum_scatter(
        split_product(out_cotangent, reduced, (((0,), (0,)), ((), ()))),
        "fs",
        scatter_dimension=0,
        tiled=True,
    )
    proj_rows = lax.psum_scatter(proj_rows, "tp", scatter_dimension=1, tiled=True)
    projected = lax.psum(proj_rows, "rep")
    first_new = beta_first * first_moment + (1.0 - beta_first) * projected
    second_new = beta_second * second_moment + (1.0 - beta_second) * projected * projected
    direction = first_new / (jnp.sqrt(second_new) + 1e-08)
    energy = lax.psum(jnp.sum(direction * direction), ("fs", "tp"))
    entries = direction.shape[0] * direction.shape[1] * lax.axis_size("fs") * lax.axis_size("tp")
    spread = jnp.sqrt(energy / entries)
    full_direction = lax.all_gather(direction, "tp", axis=1, tiled=True)
    step_out = split_product(basis, full_direction, (((1,), (1,)), ((), ()))) * (
        -1.0 / (spread + 1e-06)
    )
    weight_new = weight + step_out
    weight_copy = lax.all_gather(weight_new.astype(jnp.bfloat16), "fs", axis=1, tiled=True)
    return (weight_new, weight_copy, step_out, first_new, second_new)


def exchange_kernel(
    axes,
    lambda_ref,
    gain_ref,
    first_hbm,
    second_hbm,
    cot_hbm,
    basis_hbm,
    weight_hbm,
    moment1_hbm,
    moment2_hbm,
    gathered_out,
    direction_out,
    projected_out,
    first_v,
    second_v,
    cot_v,
    basis_v,
    weight_v,
    narrow_v,
    moment1_v,
    moment2_v,
    turned_v,
    mine_v,
    pair_send_v,
    pair_recv_v,
    plane_send_v,
    plane_recv_v,
    total_v,
    line_send_v,
    line_recv_v,
    projected_v,
    direction_v,
    load_sem,
    tile_sem,
    wz_send,
    wz_recv,
    wp_send,
    wp_recv,
    pair_send,
    pair_recv,
    plane_send,
    plane_recv,
    line_send,
    line_recv,
    proj_send,
    proj_recv,
    dz_send,
    dz_recv,
    dp_send,
    dp_recv,
    dt_send,
    dt_recv,
):
    line, plane = axes
    fs, rep, tp = lax.axis_index("fs"), lax.axis_index("rep"), lax.axis_index("tp")
    other = 1 - tp
    tokens, width = cot_v.shape
    half = direction_v.shape[-1]
    quarter = direction_v.shape[-2]
    shard = weight_v.shape[1]
    weight_rows = weight_v.shape[0]
    head_width = gain_ref.shape[1]
    heads = first_v.shape[1] // head_width
    tiles = tile_sem.shape[0]
    tile = tokens // tiles

    def ahead(at, step, count):
        return lax.rem(at + 1 + step, count)

    def behind(at, step, count):
        return lax.rem(at + count - 1 - step, count)

    def remote(source, target, send, recv, where):
        return pltpu.make_async_remote_copy(
            src_ref=source,
            dst_ref=target,
            send_sem=send,
            recv_sem=recv,
            device_id=where,
            device_id_type=MESH,
        )

    my_rows = pl.ds(pl.multiple_of(rep * weight_rows, weight_rows), weight_rows)
    my_quarter = pl.ds(pl.multiple_of(rep * quarter, quarter), quarter)

    loads = [
        pltpu.make_async_copy(weight_hbm.at[my_rows], weight_v, load_sem.at[0]),
        pltpu.make_async_copy(
            basis_hbm.at[:, pl.ds(pl.multiple_of(tp * half, half), half)],
            basis_v.at[:, pl.ds(0, half)],
            load_sem.at[1],
        ),
        pltpu.make_async_copy(
            basis_hbm.at[:, pl.ds(pl.multiple_of(other * half, half), half)],
            basis_v.at[:, pl.ds(half, half)],
            load_sem.at[2],
        ),
        pltpu.make_async_copy(cot_hbm, cot_v, load_sem.at[3]),
        pltpu.make_async_copy(moment1_hbm.at[my_quarter], moment1_v, load_sem.at[4]),
        pltpu.make_async_copy(moment2_hbm.at[my_quarter], moment2_v, load_sem.at[5]),
    ]
    loads[0].start()
    loads[1].start()
    loads[2].start()
    tile_loads = []
    for t in range(tiles):
        rows = pl.ds(t * tile, tile)
        pieces = (
            pltpu.make_async_copy(first_hbm.at[rows], first_v.at[rows], tile_sem.at[t, 0]),
            pltpu.make_async_copy(second_hbm.at[rows], second_v.at[rows], tile_sem.at[t, 1]),
        )
        for piece in pieces:
            piece.start()
        tile_loads.append(pieces)
    for load in loads[3:]:
        load.start()

    barrier = pltpu.get_barrier_semaphore()
    for step in range(line - 1):
        pl.semaphore_signal(
            barrier, inc=1, device_id={"fs": ahead(fs, step, line)}, device_id_type=MESH
        )
    for step in range(plane - 1):
        pl.semaphore_signal(
            barrier, inc=1, device_id={"rep": ahead(rep, step, plane)}, device_id_type=MESH
        )
    pl.semaphore_signal(barrier, inc=1, device_id={"tp": other}, device_id_type=MESH)
    pl.semaphore_wait(barrier, line + plane - 1)

    sends = []
    receives = []

    loads[0].wait()
    narrow_v[...] = weight_v[...].astype(jnp.bfloat16)
    weight_line = []
    for step in range(line - 1):
        copy = remote(
            narrow_v,
            gathered_out.at[fs, my_rows],
            wz_send.at[step],
            wz_recv.at[step],
            {"fs": ahead(fs, step, line)},
        )
        copy.start()
        weight_line.append(copy)
        sends.append(copy)

    def pass_on(step):
        weight_line[step].wait_recv()
        source = behind(fs, step, line)
        for to in range(plane - 1):
            copy = remote(
                gathered_out.at[source, my_rows],
                gathered_out.at[source, my_rows],
                wp_send.at[step, to],
                wp_recv.at[step, to],
                {"rep": ahead(rep, to, plane)},
            )
            copy.start()
            sends.append(copy)
            receives.append(copy)

    loads[1].wait()
    loads[2].wait()
    gain = gain_ref[...] * out_scale
    for t in range(tiles):
        for piece in tile_loads[t]:
            piece.wait()
        rows = pl.ds(t * tile, tile)
        reduced = None
        for h in range(heads):
            lanes = pl.ds(h * head_width, head_width)
            mixture = first_v[rows, lanes].astype(jnp.float32) - lambda_ref[h] * second_v[
                rows, lanes
            ].astype(jnp.float32)
            inverse = lax.rsqrt(jnp.mean(mixture * mixture, axis=-1, keepdims=True) + 1e-06)
            normed = (mixture * inverse * gain).astype(jnp.bfloat16)
            term = jnp.dot(normed, basis_v[lanes, :], preferred_element_type=jnp.float32)
            reduced = term if reduced is None else reduced + term
        turned_v[:, rows] = reduced.T.astype(jnp.bfloat16)

    loads[3].wait()
    pair_copies = []
    plane_copies = []

    def pair_sum(step):
        pair_copies[step].wait_recv()
        return mine_v[step] + pair_recv_v[step]

    def send_plane(step):
        plane_send_v[step] = pair_sum(step).astype(jnp.bfloat16)
        copy = remote(
            plane_send_v.at[step],
            plane_recv_v.at[step],
            plane_send.at[step],
            plane_recv.at[step],
            {"rep": ahead(rep, step, plane)},
        )
        copy.start()
        plane_copies.append(copy)
        sends.append(copy)

    for step in range(plane):
        part = ahead(rep, step, plane)
        for at in range(line):
            start = pl.multiple_of(at * shard + part * quarter, quarter)
            product = jnp.dot(
                turned_v[...], cot_v[:, pl.ds(start, quarter)], preferred_element_type=jnp.float32
            )
            mine_v[step, at] = product[:half].T
            pair_send_v[step, at] = product[half:].T
        copy = remote(
            pair_send_v.at[step],
            pair_recv_v.at[step],
            pair_send.at[step],
            pair_recv.at[step],
            {"tp": other},
        )
        copy.start()
        pair_copies.append(copy)
        sends.append(copy)
        if step > 0:
            send_plane(step - 1)

    pass_on(0)
    total = pair_sum(plane - 1)
    for step in range(plane - 1):
        plane_copies[step].wait_recv()
        total = total + plane_recv_v[step].astype(jnp.float32)
    total_v[...] = total
    line_send_v[...] = total.astype(jnp.bfloat16)
    line_copies = []
    for step in range(line - 1):
        to = ahead(fs, step, line)
        copy = remote(
            line_send_v.at[to],
            line_recv_v.at[step],
            line_send.at[step],
            line_recv.at[step],
            {"fs": to},
        )
        copy.start()
        line_copies.append(copy)
        sends.append(copy)
    for step in range(1, line - 2):
        pass_on(step)
    projected = total_v[fs]
    for step in range(line - 1):
        line_copies[step].wait_recv()
        projected = projected + line_recv_v[step].astype(jnp.float32)
    projected_v[rep] = projected
    loads[4].wait()
    loads[5].wait()
    first_new = beta_first * moment1_v[...] + (1.0 - beta_first) * projected
    second_new = beta_second * moment2_v[...] + (1.0 - beta_second) * projected * projected
    direction = first_new / (jnp.sqrt(second_new) + 1e-08)
    direction_v[tp, fs, rep] = direction.astype(jnp.bfloat16)
    direction_line = []
    for step in range(line - 1):
        here = direction_v.at[tp, fs, rep]
        copy = remote(
            here, here, dz_send.at[step], dz_recv.at[step], {"fs": ahead(fs, step, line)}
        )
        copy.start()
        direction_line.append(copy)
        sends.append(copy)
    for step in range(plane - 1):
        here = projected_v.at[rep]
        copy = remote(
            here, here, proj_send.at[step], proj_recv.at[step], {"rep": ahead(rep, step, plane)}
        )
        copy.start()
        sends.append(copy)
        receives.append(copy)
    for step in range(max(1, line - 2), line - 1):
        pass_on(step)
    for copy in direction_line:
        copy.wait_recv()
    direction_plane = []
    for step in range(plane - 1):
        here = direction_v.at[tp, :, rep]
        copy = remote(
            here, here, dp_send.at[step], dp_recv.at[step], {"rep": ahead(rep, step, plane)}
        )
        copy.start()
        direction_plane.append(copy)
        sends.append(copy)

    def to_pair(step, part):
        here = direction_v.at[tp, :, part]
        copy = remote(here, here, dt_send.at[step], dt_recv.at[step], {"tp": other})
        copy.start()
        sends.append(copy)
        receives.append(copy)

    to_pair(plane - 1, rep)
    for step in range(plane - 1):
        direction_plane[step].wait_recv()
        to_pair(step, behind(rep, step, plane))
    for copy in receives:
        copy.wait_recv()
    outs = [
        pltpu.make_async_copy(direction_v, direction_out, load_sem.at[0]),
        pltpu.make_async_copy(projected_v, projected_out, load_sem.at[1]),
    ]
    for copy in outs:
        copy.start()
    for copy in sends:
        copy.wait_send()
    for copy in outs:
        copy.wait()


def update_kernel(
    line,
    basis_ref,
    direction_ref,
    projected_ref,
    moment1_ref,
    moment2_ref,
    weight_ref,
    gathered_ref,
    weight_new_ref,
    copy_ref,
    step_ref,
    first_new_ref,
    second_new_ref,
    scale_ref,
    joined_ref,
):
    fs = lax.axis_index("fs")
    shard = weight_ref.shape[1]

    @pl.when(pl.program_id(0) == 0)
    def _():
        projected = projected_ref[...]
        first_new_ref[...] = beta_first * moment1_ref[...] + (1.0 - beta_first) * projected
        second_new_ref[...] = (
            beta_second * moment2_ref[...] + (1.0 - beta_second) * projected * projected
        )
        half = direction_ref.shape[-1]
        energy = jnp.zeros((1, half), jnp.float32)
        for side in range(direction_ref.shape[0]):
            piece = direction_ref[side]
            joined_ref[:, side * half : (side + 1) * half] = piece
            wide = piece.astype(jnp.float32)
            energy += jnp.sum(wide * wide, axis=0, keepdims=True)
        entries = joined_ref.shape[0] * joined_ref.shape[1]
        spread = jnp.sqrt(jnp.sum(energy, axis=1, keepdims=True) / entries)
        scale_ref[...] = jnp.broadcast_to(-1.0 / (spread + 1e-06), scale_ref.shape)

    scale = scale_ref[0:1, 0:1]
    basis = basis_ref[...]
    for at in range(line):
        columns = pl.ds(at * shard, shard)
        step = (
            lax.dot_general(
                basis,
                joined_ref[columns, :],
                (((1,), (1,)), ((), ())),
                preferred_element_type=jnp.float32,
            )
            * scale
        )

        @pl.when(fs == at)
        def _():
            fresh = weight_ref[...] + step
            step_ref[...] = step
            weight_new_ref[...] = fresh
            copy_ref[:, columns] = fresh.astype(jnp.bfloat16)

        @pl.when(fs != at)
        def _():
            copy_ref[:, columns] = (gathered_ref[at].astype(jnp.float32) + step).astype(
                jnp.bfloat16
            )


def fast_body(
    sizes,
    first_mix,
    second_mix,
    lambda_head,
    head_gain,
    out_cotangent,
    basis,
    weight,
    first_moment,
    second_moment,
):
    line, plane = sizes
    tokens, width = out_cotangent.shape
    values, rank = basis.shape
    shard, half = first_moment.shape
    quarter = shard // plane
    rows = values // plane
    tile = 256 if tokens % 256 == 0 else tokens
    tiles = tokens // tile
    any_space = pl.BlockSpec(memory_space=pl.ANY)
    dma = pltpu.SemaphoreType.DMA
    f32, bf16 = jnp.float32, jnp.bfloat16
    gathered, direction, projected = pl.pallas_call(
        functools.partial(exchange_kernel, sizes),
        out_shape=(
            jax.ShapeDtypeStruct((line, values, shard), bf16),
            jax.ShapeDtypeStruct((2, line, plane, quarter, half), bf16),
            jax.ShapeDtypeStruct((plane, quarter, half), f32),
        ),
        in_specs=[
            pl.BlockSpec(memory_space=pltpu.SMEM),
            pl.BlockSpec(memory_space=pltpu.VMEM),
        ]
        + [any_space] * 7,
        out_specs=(any_space,) * 3,
        scratch_shapes=[
            pltpu.VMEM(first_mix.shape, bf16),
            pltpu.VMEM(second_mix.shape, bf16),
            pltpu.VMEM(out_cotangent.shape, bf16),
            pltpu.VMEM(basis.shape, bf16),
            pltpu.VMEM((rows, shard), f32),
            pltpu.VMEM((rows, shard), bf16),
            pltpu.VMEM((quarter, half), f32),
            pltpu.VMEM((quarter, half), f32),
            pltpu.VMEM((rank, tokens), bf16),
            pltpu.VMEM((plane, line, quarter, half), f32),
            pltpu.VMEM((plane, line, quarter, half), f32),
            pltpu.VMEM((plane, line, quarter, half), f32),
            pltpu.VMEM((plane - 1, line, quarter, half), bf16),
            pltpu.VMEM((plane - 1, line, quarter, half), bf16),
            pltpu.VMEM((line, quarter, half), f32),
            pltpu.VMEM((line, quarter, half), bf16),
            pltpu.VMEM((line - 1, quarter, half), bf16),
            pltpu.VMEM((plane, quarter, half), f32),
            pltpu.VMEM((2, line, plane, quarter, half), bf16),
            dma((6,)),
            dma((tiles, 2)),
            dma((line - 1,)),
            dma((line - 1,)),
            dma((line - 1, plane - 1)),
            dma((line - 1, plane - 1)),
            dma((plane,)),
            dma((plane,)),
            dma((plane - 1,)),
            dma((plane - 1,)),
            dma((line - 1,)),
            dma((line - 1,)),
            dma((plane - 1,)),
            dma((plane - 1,)),
            dma((line - 1,)),
            dma((line - 1,)),
            dma((plane - 1,)),
            dma((plane - 1,)),
            dma((plane,)),
            dma((plane,)),
        ],
        compiler_params=pltpu.CompilerParams(
            collective_id=0, has_side_effects=True, vmem_limit_bytes=vmem_grant
        ),
    )(
        lambda_head,
        head_gain.reshape(1, -1),
        first_mix,
        second_mix,
        out_cotangent,
        basis,
        weight,
        first_moment,
        second_moment,
    )
    block = values // 4
    whole = lambda *shape: pl.BlockSpec(shape, lambda i: (0,) * len(shape))
    rowed = lambda columns: pl.BlockSpec((block, columns), lambda i: (i, 0))
    return pl.pallas_call(
        functools.partial(update_kernel, line),
        grid=(values // block,),
        out_shape=(
            jax.ShapeDtypeStruct(weight.shape, f32),
            jax.ShapeDtypeStruct((values, width), bf16),
            jax.ShapeDtypeStruct(weight.shape, f32),
            jax.ShapeDtypeStruct(first_moment.shape, f32),
            jax.ShapeDtypeStruct(first_moment.shape, f32),
        ),
        in_specs=[
            rowed(rank),
            whole(2, width, half),
            whole(shard, half),
            whole(shard, half),
            whole(shard, half),
            rowed(shard),
            pl.BlockSpec((line, block, shard), lambda i: (0, i, 0)),
        ],
        out_specs=(
            rowed(shard),
            rowed(width),
            rowed(shard),
            whole(shard, half),
            whole(shard, half),
        ),
        scratch_shapes=[pltpu.VMEM((8, 128), f32), pltpu.VMEM((width, rank), bf16)],
        compiler_params=pltpu.CompilerParams(vmem_limit_bytes=vmem_grant),
    )(
        basis,
        direction.reshape(2, width, half),
        projected.reshape(shard, half),
        first_moment,
        second_moment,
        weight,
        gathered,
    )


def solution(mesh):
    line, plane, pair = (mesh.shape[name] for name in ("fs", "rep", "tp"))

    def chosen(*args):
        basis, first_moment = args[5], args[7]
        quarter_fits = first_moment.shape[0] % (plane * 128) == 0
        rows_fit = basis.shape[0] % (plane * 16) == 0 and basis.shape[0] % 64 == 0
        rank_fits = pair == 2 and first_moment.shape[1] % 128 == 0
        if min(line, plane) > 1 and quarter_fits and rows_fit and rank_fits:
            return fast_body((line, plane), *args)
        return body(*args)

    return jax.shard_map(
        chosen,
        mesh=mesh,
        in_specs=(
            P(("fs", "rep"), "tp"),
            P(("fs", "rep"), "tp"),
            P("tp"),
            P(),
            P(("fs", "rep"), None),
            P("tp", None),
            P("tp", "fs"),
            P("fs", "tp"),
            P("fs", "tp"),
        ),
        out_specs=(P("tp", "fs"), P("tp", None), P("tp", "fs"), P("fs", "tp"), P("fs", "tp")),
        check_vma=False,
    )
```

```python
import functools

import jax
import jax.numpy as jnp
from jax import lax
from jax.experimental import pallas as pl
from jax.experimental.pallas import tpu as pltpu
from jax.sharding import PartitionSpec as P

MESH = pl.DeviceIdType.MESH

vmem_grant = 67043328
out_scale = 0.8
beta_first = 0.9
beta_second = 0.95


def head_output(first_piece, second_piece, lambdas, head_gain):
    token_count = first_piece.shape[0]
    head_width = head_gain.shape[0]
    head_count = lambdas.shape[0] // head_width
    mixture = first_piece.astype(jnp.float32) - lambdas[None, :] * second_piece.astype(jnp.float32)
    grouped = mixture.reshape(token_count, head_count, head_width)
    inverse = lax.rsqrt(jnp.mean(grouped * grouped, axis=-1, keepdims=True) + 1e-06)
    normed = grouped * inverse * head_gain[None, None, :] * out_scale
    return normed.reshape(token_count, head_count * head_width).astype(jnp.bfloat16)


def split_product(narrow, wide, numbers):
    upper = wide.astype(jnp.bfloat16)
    lower = (wide - upper.astype(jnp.float32)).astype(jnp.bfloat16)
    return lax.dot_general(
        narrow, upper, numbers, preferred_element_type=jnp.float32
    ) + lax.dot_general(narrow, lower, numbers, preferred_element_type=jnp.float32)


def body(
    first_mix,
    second_mix,
    lambda_head,
    head_gain,
    out_cotangent,
    basis,
    weight,
    first_moment,
    second_moment,
):
    lambdas = jnp.repeat(lambda_head, head_gain.shape[0])
    head_out = head_output(first_mix, second_mix, lambdas, head_gain)
    reduced = jnp.dot(head_out, basis, preferred_element_type=jnp.float32)
    proj_rows = lax.psum_scatter(
        split_product(out_cotangent, reduced, (((0,), (0,)), ((), ()))),
        "fs",
        scatter_dimension=0,
        tiled=True,
    )
    proj_rows = lax.psum_scatter(proj_rows, "tp", scatter_dimension=1, tiled=True)
    projected = lax.psum(proj_rows, "rep")
    first_new = beta_first * first_moment + (1.0 - beta_first) * projected
    second_new = beta_second * second_moment + (1.0 - beta_second) * projected * projected
    direction = first_new / (jnp.sqrt(second_new) + 1e-08)
    energy = lax.psum(jnp.sum(direction * direction), ("fs", "tp"))
    entries = direction.shape[0] * direction.shape[1] * lax.axis_size("fs") * lax.axis_size("tp")
    spread = jnp.sqrt(energy / entries)
    full_direction = lax.all_gather(direction, "tp", axis=1, tiled=True)
    step_out = split_product(basis, full_direction, (((1,), (1,)), ((), ()))) * (
        -1.0 / (spread + 1e-06)
    )
    weight_new = weight + step_out
    weight_copy = lax.all_gather(weight_new.astype(jnp.bfloat16), "fs", axis=1, tiled=True)
    return (weight_new, weight_copy, step_out, first_new, second_new)


def exchange_kernel(
    axes,
    lambda_ref,
    gain_ref,
    first_hbm,
    second_hbm,
    cot_hbm,
    basis_hbm,
    weight_hbm,
    moment1_hbm,
    moment2_hbm,
    gathered_out,
    direction_out,
    projected_out,
    scale_out,
    first_v,
    second_v,
    cot_v,
    basis_v,
    weight_v,
    narrow_v,
    moment1_v,
    moment2_v,
    turned_v,
    mine_v,
    pair_send_v,
    pair_recv_v,
    plane_send_v,
    plane_recv_v,
    total_v,
    line_send_v,
    line_recv_v,
    projected_v,
    direction_v,
    joined_v,
    scale_v,
    load_sem,
    tile_sem,
    wz_send,
    wz_recv,
    wp_send,
    wp_recv,
    pair_send,
    pair_recv,
    plane_send,
    plane_recv,
    line_send,
    line_recv,
    proj_send,
    proj_recv,
    dz_send,
    dz_recv,
    dp_send,
    dp_recv,
    dt_send,
    dt_recv,
):
    line, plane = axes
    fs, rep, tp = lax.axis_index("fs"), lax.axis_index("rep"), lax.axis_index("tp")
    other = 1 - tp
    tokens, width = cot_v.shape
    half = direction_v.shape[-1]
    quarter = direction_v.shape[-2]
    shard = weight_v.shape[1]
    weight_rows = weight_v.shape[0]
    head_width = gain_ref.shape[1]
    heads = first_v.shape[1] // head_width
    tiles = tile_sem.shape[0]
    tile = tokens // tiles

    def ahead(at, step, count):
        return lax.rem(at + 1 + step, count)

    def behind(at, step, count):
        return lax.rem(at + count - 1 - step, count)

    fast_side = rep + 1 - 2 * lax.rem(rep, 2)
    slow_side = lax.rem(rep + 2, 4)
    peers = (3 - rep, slow_side, fast_side, rep)

    def remote(source, target, send, recv, where):
        return pltpu.make_async_remote_copy(
            src_ref=source,
            dst_ref=target,
            send_sem=send,
            recv_sem=recv,
            device_id=where,
            device_id_type=MESH,
        )

    my_rows = pl.ds(pl.multiple_of(rep * weight_rows, weight_rows), weight_rows)
    my_quarter = pl.ds(pl.multiple_of(rep * quarter, quarter), quarter)

    loads = [
        pltpu.make_async_copy(weight_hbm.at[my_rows], weight_v, load_sem.at[0]),
        pltpu.make_async_copy(
            basis_hbm.at[:, pl.ds(pl.multiple_of(tp * half, half), half)],
            basis_v.at[:, pl.ds(0, half)],
            load_sem.at[1],
        ),
        pltpu.make_async_copy(
            basis_hbm.at[:, pl.ds(pl.multiple_of(other * half, half), half)],
            basis_v.at[:, pl.ds(half, half)],
            load_sem.at[2],
        ),
        pltpu.make_async_copy(cot_hbm, cot_v, load_sem.at[3]),
        pltpu.make_async_copy(moment1_hbm.at[my_quarter], moment1_v, load_sem.at[4]),
        pltpu.make_async_copy(moment2_hbm.at[my_quarter], moment2_v, load_sem.at[5]),
    ]
    loads[0].start()
    loads[1].start()
    loads[2].start()
    tile_loads = []
    for t in range(tiles):
        rows = pl.ds(t * tile, tile)
        pieces = (
            pltpu.make_async_copy(first_hbm.at[rows], first_v.at[rows], tile_sem.at[t, 0]),
            pltpu.make_async_copy(second_hbm.at[rows], second_v.at[rows], tile_sem.at[t, 1]),
        )
        for piece in pieces:
            piece.start()
        tile_loads.append(pieces)
    for load in loads[3:]:
        load.start()

    barrier = pltpu.get_barrier_semaphore()
    for step in range(line - 1):
        pl.semaphore_signal(
            barrier, inc=1, device_id={"fs": ahead(fs, step, line)}, device_id_type=MESH
        )
    for step in range(plane - 1):
        pl.semaphore_signal(
            barrier, inc=1, device_id={"rep": peers[step]}, device_id_type=MESH
        )
    pl.semaphore_signal(barrier, inc=1, device_id={"tp": other}, device_id_type=MESH)
    pl.semaphore_wait(barrier, line + plane - 1)

    sends = []
    receives = []
    pair_receives = []
    proj_receives = []

    loads[0].wait()
    narrow_v[...] = weight_v[...].astype(jnp.bfloat16)
    weight_line = {}

    def send_line(step):
        copy = remote(
            narrow_v,
            gathered_out.at[fs, my_rows],
            wz_send.at[step],
            wz_recv.at[step],
            {"fs": ahead(fs, step, line)},
        )
        copy.start()
        weight_line[step] = copy
        sends.append(copy)

    early = (0, line - 2)
    late = tuple(range(1, line - 2))
    for step in early:
        send_line(step)

    side_copies = {}

    def pass_on(step):
        weight_line[step].wait_recv()
        here = gathered_out.at[behind(fs, step, line), my_rows]
        for side, peer in enumerate((slow_side, fast_side)):
            copy = remote(
                here, here, wp_send.at[step, side], wp_recv.at[step, side], {"rep": peer}
            )
            copy.start()
            sends.append(copy)
            side_copies[step, side] = copy

    def relay(step):
        source = behind(fs, step, line)
        part = weight_rows // 2
        for side, (origin, peer) in enumerate(((slow_side, fast_side), (fast_side, slow_side))):
            side_copies[step, side].wait_recv()
            start = pl.multiple_of(origin * weight_rows + side * part, part)
            here = gathered_out.at[source, pl.ds(start, part)]
            copy = remote(
                here, here, wp_send.at[step, 2 + side], wp_recv.at[step, 2 + side], {"rep": peer}
            )
            copy.start()
            sends.append(copy)
            receives.append(copy)

    loads[1].wait()
    loads[2].wait()
    gain = gain_ref[...] * out_scale
    for t in range(tiles):
        for piece in tile_loads[t]:
            piece.wait()
        rows = pl.ds(t * tile, tile)
        reduced = None
        for h in range(heads):
            lanes = pl.ds(h * head_width, head_width)
            mixture = first_v[rows, lanes].astype(jnp.float32) - lambda_ref[h] * second_v[
                rows, lanes
            ].astype(jnp.float32)
            inverse = lax.rsqrt(jnp.mean(mixture * mixture, axis=-1, keepdims=True) + 1e-06)
            normed = (mixture * inverse * gain).astype(jnp.bfloat16)
            term = jnp.dot(normed, basis_v[lanes, :], preferred_element_type=jnp.float32)
            reduced = term if reduced is None else reduced + term
        turned_v[:, rows] = reduced.T.astype(jnp.bfloat16)

    loads[3].wait()
    pair_copies = []
    plane_copies = []

    def pair_sum(step):
        pair_copies[step].wait_recv()
        return mine_v[step] + pair_recv_v[step]

    def send_plane(step):
        plane_send_v[step] = pair_sum(step).astype(jnp.bfloat16)
        copy = remote(
            plane_send_v.at[step],
            plane_recv_v.at[step],
            plane_send.at[step],
            plane_recv.at[step],
            {"rep": peers[step]},
        )
        copy.start()
        plane_copies.append(copy)
        sends.append(copy)

    for step in range(plane):
        part = peers[step]
        for at in range(line):
            start = pl.multiple_of(at * shard + part * quarter, quarter)
            product = jnp.dot(
                turned_v[...], cot_v[:, pl.ds(start, quarter)], preferred_element_type=jnp.float32
            )
            mine_v[step, at] = product[:half].T
            pair_send_v[step, at] = product[half:].T
        copy = remote(
            pair_send_v.at[step],
            pair_recv_v.at[step],
            pair_send.at[step],
            pair_recv.at[step],
            {"tp": other},
        )
        copy.start()
        pair_copies.append(copy)
        sends.append(copy)
        if step > 0:
            send_plane(step - 1)

    pass_on(0)
    total = pair_sum(plane - 1)
    for step in range(plane - 1):
        plane_copies[step].wait_recv()
        total = total + plane_recv_v[step].astype(jnp.float32)
    total_v[...] = total
    line_send_v[...] = total.astype(jnp.bfloat16)
    line_copies = []
    for step in range(line - 1):
        to = ahead(fs, step, line)
        copy = remote(
            line_send_v.at[to],
            line_recv_v.at[step],
            line_send.at[step],
            line_recv.at[step],
            {"fs": to},
        )
        copy.start()
        line_copies.append(copy)
        sends.append(copy)
    relay(0)
    pass_on(line - 2)
    projected = total_v[fs]
    for step in range(line - 1):
        line_copies[step].wait_recv()
        projected = projected + line_recv_v[step].astype(jnp.float32)
    projected_v[rep] = projected
    loads[4].wait()
    loads[5].wait()
    first_new = beta_first * moment1_v[...] + (1.0 - beta_first) * projected
    second_new = beta_second * moment2_v[...] + (1.0 - beta_second) * projected * projected
    direction = first_new / (jnp.sqrt(second_new) + 1e-08)
    direction_v[tp, fs, rep] = direction.astype(jnp.bfloat16)
    direction_line = []
    for step in range(line - 1):
        here = direction_v.at[tp, fs, rep]
        copy = remote(
            here, here, dz_send.at[step], dz_recv.at[step], {"fs": ahead(fs, step, line)}
        )
        copy.start()
        direction_line.append(copy)
        sends.append(copy)
    for step in late:
        send_line(step)
    for step in range(plane - 1):
        here = projected_v.at[rep]
        copy = remote(
            here, here, proj_send.at[step], proj_recv.at[step], {"rep": peers[step]}
        )
        copy.start()
        sends.append(copy)
        proj_receives.append(copy)
    for copy in direction_line:
        copy.wait_recv()
    direction_plane = []
    for step in range(plane - 1):
        here = direction_v.at[tp, :, rep]
        copy = remote(
            here, here, dp_send.at[step], dp_recv.at[step], {"rep": peers[step]}
        )
        copy.start()
        direction_plane.append(copy)
        sends.append(copy)

    def to_pair(step, part):
        here = direction_v.at[tp, :, part]
        copy = remote(here, here, dt_send.at[step], dt_recv.at[step], {"tp": other})
        copy.start()
        sends.append(copy)
        pair_receives.append(copy)

    to_pair(plane - 1, rep)
    for step in range(plane - 1):
        direction_plane[step].wait_recv()
        to_pair(step, peers[step])
    relay(line - 2)
    for step in late:
        pass_on(step)
    for copy in pair_receives:
        copy.wait_recv()
    energy = jnp.zeros((1, half), jnp.float32)
    for side in range(2):
        piece = direction_v[side].reshape(width, half)
        wide = piece.astype(jnp.float32)
        joined_v[side * half : (side + 1) * half, :] = wide.T.astype(jnp.bfloat16)
        energy += jnp.sum(wide * wide, axis=0, keepdims=True)
    spread = jnp.sqrt(jnp.sum(energy, axis=1, keepdims=True) / (width * 2 * half))
    scale_v[...] = jnp.broadcast_to(-1.0 / (spread + 1e-06), scale_v.shape)
    for step in late:
        relay(step)
    for copy in proj_receives:
        copy.wait_recv()
    outs = [
        pltpu.make_async_copy(joined_v, direction_out, load_sem.at[0]),
        pltpu.make_async_copy(projected_v, projected_out, load_sem.at[1]),
        pltpu.make_async_copy(scale_v, scale_out, load_sem.at[2]),
    ]
    for copy in outs:
        copy.start()
    for copy in receives:
        copy.wait_recv()
    for copy in sends:
        copy.wait_send()
    for copy in outs:
        copy.wait()


def update_kernel(
    line,
    basis_ref,
    direction_ref,
    scale_ref,
    projected_ref,
    moment1_ref,
    moment2_ref,
    weight_ref,
    gathered_ref,
    weight_new_ref,
    copy_ref,
    step_ref,
    first_new_ref,
    second_new_ref,
):
    fs = lax.axis_index("fs")
    shard = weight_ref.shape[1]
    projected = projected_ref[...]
    first_new_ref[...] = beta_first * moment1_ref[...] + (1.0 - beta_first) * projected
    second_new_ref[...] = (
        beta_second * moment2_ref[...] + (1.0 - beta_second) * projected * projected
    )
    scale = scale_ref[0:1, 0:1]
    basis = basis_ref[...]
    for at in range(line):
        columns = pl.ds(at * shard, shard)
        step = (
            jnp.dot(basis, direction_ref[:, columns], preferred_element_type=jnp.float32)
            * scale
        )

        @pl.when(fs == at)
        def _():
            fresh = weight_ref[...] + step
            step_ref[...] = step
            weight_new_ref[...] = fresh
            copy_ref[:, columns] = fresh.astype(jnp.bfloat16)

        @pl.when(fs != at)
        def _():
            copy_ref[:, columns] = (gathered_ref[at].astype(jnp.float32) + step).astype(
                jnp.bfloat16
            )


def fast_body(
    sizes,
    first_mix,
    second_mix,
    lambda_head,
    head_gain,
    out_cotangent,
    basis,
    weight,
    first_moment,
    second_moment,
):
    line, plane = sizes
    tokens, width = out_cotangent.shape
    values, rank = basis.shape
    shard, half = first_moment.shape
    quarter = shard // plane
    rows = values // plane
    tile = 256 if tokens % 256 == 0 else tokens
    tiles = tokens // tile
    any_space = pl.BlockSpec(memory_space=pl.ANY)
    dma = pltpu.SemaphoreType.DMA
    f32, bf16 = jnp.float32, jnp.bfloat16
    gathered, direction, projected, scale = pl.pallas_call(
        functools.partial(exchange_kernel, sizes),
        out_shape=(
            jax.ShapeDtypeStruct((line, values, shard), bf16),
            jax.ShapeDtypeStruct((rank, width), bf16),
            jax.ShapeDtypeStruct((plane, quarter, half), f32),
            jax.ShapeDtypeStruct((8, 128), f32),
        ),
        in_specs=[
            pl.BlockSpec(memory_space=pltpu.SMEM),
            pl.BlockSpec(memory_space=pltpu.VMEM),
        ]
        + [any_space] * 7,
        out_specs=(any_space,) * 4,
        scratch_shapes=[
            pltpu.VMEM(first_mix.shape, bf16),
            pltpu.VMEM(second_mix.shape, bf16),
            pltpu.VMEM(out_cotangent.shape, bf16),
            pltpu.VMEM(basis.shape, bf16),
            pltpu.VMEM((rows, shard), f32),
            pltpu.VMEM((rows, shard), bf16),
            pltpu.VMEM((quarter, half), f32),
            pltpu.VMEM((quarter, half), f32),
            pltpu.VMEM((rank, tokens), bf16),
            pltpu.VMEM((plane, line, quarter, half), f32),
            pltpu.VMEM((plane, line, quarter, half), f32),
            pltpu.VMEM((plane, line, quarter, half), f32),
            pltpu.VMEM((plane - 1, line, quarter, half), bf16),
            pltpu.VMEM((plane - 1, line, quarter, half), bf16),
            pltpu.VMEM((line, quarter, half), f32),
            pltpu.VMEM((line, quarter, half), bf16),
            pltpu.VMEM((line - 1, quarter, half), bf16),
            pltpu.VMEM((plane, quarter, half), f32),
            pltpu.VMEM((2, line, plane, quarter, half), bf16),
            pltpu.VMEM((rank, width), bf16),
            pltpu.VMEM((8, 128), f32),
            dma((6,)),
            dma((tiles, 2)),
            dma((line - 1,)),
            dma((line - 1,)),
            dma((line - 1, 4)),
            dma((line - 1, 4)),
            dma((plane,)),
            dma((plane,)),
            dma((plane - 1,)),
            dma((plane - 1,)),
            dma((line - 1,)),
            dma((line - 1,)),
            dma((plane - 1,)),
            dma((plane - 1,)),
            dma((line - 1,)),
            dma((line - 1,)),
            dma((plane - 1,)),
            dma((plane - 1,)),
            dma((plane,)),
            dma((plane,)),
        ],
        compiler_params=pltpu.CompilerParams(
            collective_id=0, has_side_effects=True, vmem_limit_bytes=vmem_grant
        ),
    )(
        lambda_head,
        head_gain.reshape(1, -1),
        first_mix,
        second_mix,
        out_cotangent,
        basis,
        weight,
        first_moment,
        second_moment,
    )
    blocks = 2
    block = values // blocks
    moment_block = shard // blocks
    whole = lambda *shape: pl.BlockSpec(shape, lambda i: (0,) * len(shape))
    mrow = pl.BlockSpec((moment_block, half), lambda i: (i, 0))
    rowed = lambda columns: pl.BlockSpec((block, columns), lambda i: (i, 0))
    return pl.pallas_call(
        functools.partial(update_kernel, line),
        grid=(values // block,),
        out_shape=(
            jax.ShapeDtypeStruct(weight.shape, f32),
            jax.ShapeDtypeStruct((values, width), bf16),
            jax.ShapeDtypeStruct(weight.shape, f32),
            jax.ShapeDtypeStruct(first_moment.shape, f32),
            jax.ShapeDtypeStruct(first_moment.shape, f32),
        ),
        in_specs=[
            rowed(rank),
            whole(rank, width),
            whole(8, 128),
            mrow,
            mrow,
            mrow,
            rowed(shard),
            pl.BlockSpec((line, block, shard), lambda i: (0, i, 0)),
        ],
        out_specs=(
            rowed(shard),
            rowed(width),
            rowed(shard),
            mrow,
            mrow,
        ),
        compiler_params=pltpu.CompilerParams(vmem_limit_bytes=vmem_grant),
    )(
        basis,
        direction,
        scale,
        projected.reshape(shard, half),
        first_moment,
        second_moment,
        weight,
        gathered,
    )


def solution(mesh):
    line, plane, pair = (mesh.shape[name] for name in ("fs", "rep", "tp"))

    def chosen(*args):
        basis, first_moment = args[5], args[7]
        quarter_fits = first_moment.shape[0] % (plane * 128) == 0
        rows_fit = basis.shape[0] % (plane * 16) == 0 and basis.shape[0] % 64 == 0
        rank_fits = pair == 2 and first_moment.shape[1] % 128 == 0
        if line > 2 and plane == 4 and quarter_fits and rows_fit and rank_fits:
            return fast_body((line, plane), *args)
        return body(*args)

    return jax.shard_map(
        chosen,
        mesh=mesh,
        in_specs=(
            P(("fs", "rep"), "tp"),
            P(("fs", "rep"), "tp"),
            P("tp"),
            P(),
            P(("fs", "rep"), None),
            P("tp", None),
            P("tp", "fs"),
            P("fs", "tp"),
            P("fs", "tp"),
        ),
        out_specs=(P("tp", "fs"), P("tp", None), P("tp", "fs"), P("fs", "tp"), P("fs", "tp")),
        check_vma=False,
    )
```
